32 devices in a mesh: rep: 2 (over x), fs: 8 (over z, y), tp: 2 (over core).
Axes of the slice: x: 2, y: 2, z: 4, core: 2. Of those that a mesh axis runs over, the one named last changes fastest.
Arguments:
- inputs: bfloat16 [4096, 2048], P(('rep', 'fs')), may hold values from -6 to 6
- cotangent: bfloat16 [4096, 2048], P(('rep', 'fs')), may hold values from -0.119628906 to 0.119628906
- up_weight: bfloat16 [2048, 4096], P('fs', 'tp'), may hold values from -0.125 to 0.125
- down_weight: bfloat16 [4096, 2048], P('tp', 'fs'), may hold values from -0.09375 to 0.09375
Outputs:
- grad_inputs: float32 [4096, 2048], P(('rep', 'fs'))
- grad_up: float32 [2048, 4096], P('fs', 'tp')
- grad_down: float32 [4096, 2048], P('tp', 'fs')
- norms_up: float32 [2048], P('fs')
- norms_down: float32 [4096], P('tp')
The draws below stay inside these ranges and needn't reach their ends.
All inputs are finite; a program needn't handle non-finite values.
Results may differ from the reference program's by a relative error of at most 0.0029.
Values may be sent and summed in bfloat16 or wider, within the bound.
A program may use at most 128 MiB of HBM per device.

```python
import jax
import jax.numpy as jnp
from jax import lax

D = 2048
FF = 4096
TOKENS = 4096


def spiked(array, rng, source, target, parts, factor):
    owner, partner = [(jnp.arange(array.shape[dim]) // (array.shape[dim] // parts)).reshape([-1 if axis == dim else 1 for axis in range(array.ndim)]) for dim in (source, target)]
    chosen = jax.random.permutation(rng, parts)[partner]
    strong = (owner == chosen) | (owner == (partner + parts // 2) % parts)
    return jnp.where(strong, factor * array, array)


def block_scale(own_key, shape, pieces, low, largest):
    def one(axis_at, shards_of):
        draws = jax.random.uniform(jax.random.fold_in(jax.random.fold_in(own_key, 6), axis_at), (shards_of,), jnp.float32, low / len(pieces), largest / len(pieces))
        return jnp.repeat(jnp.exp(draws), shape[axis_at] // shards_of).reshape((-1,) + (1,) * (len(shape) - axis_at - 1))

    level = one(*pieces[0])
    for cut in pieces[1:]:
        level = level * one(*cut)
    return level


def gaussian(rng, shape, spread, bound, pieces=(), held_as=jnp.bfloat16):
    array = spread * jax.random.normal(rng, shape, jnp.float32)
    if pieces:
        array = array * block_scale(rng, shape, pieces, -0.22, 0.18)
    return jnp.clip(array, -bound, bound).astype(held_as)


def noise_with(stream_key, shape, scale, bound, split, heavy, held_as=jnp.bfloat16):
    result = scale * jax.random.normal(stream_key, shape, jnp.float32)
    if split:
        result = result * block_scale(stream_key, shape, split, -0.22, 0.18)
    return jnp.clip(spiked(result, jax.random.fold_in(stream_key, 3), *heavy), -bound, bound).astype(held_as)


def setup_inputs(seed: int = 0) -> dict:
    arg_keys = jax.random.split(jax.random.key(seed), 5)
    return {
        "inputs": noise_with(arg_keys[0], (TOKENS, D), 1.0, 6.0, ((0, 16),), (0, 1, 16, 2.0)),
        "cotangent": noise_with(arg_keys[1], (TOKENS, D), 0.02, 0.119628906, ((0, 16),), (0, 1, 16, 2.0)),
        "up_weight": gaussian(arg_keys[2], (D, FF), D ** -0.5, 0.125, ((0, 8), (1, 2))),
        "down_weight": gaussian(arg_keys[3], (FF, D), FF ** -0.5, 0.09375, ((0, 2), (1, 8))),
    }


def contract(left, right, left_dim, right_dim):
    return lax.dot_general(left, right, (((left_dim,), (right_dim,)), ((), ())), preferred_element_type=jnp.float32)


def reference(inputs, cotangent, up_weight, down_weight):
    pre_act = jnp.dot(inputs, up_weight, preferred_element_type=jnp.float32)
    rectified = jnp.maximum(pre_act, 0.0)
    hidden = (rectified * rectified).astype(jnp.bfloat16)
    act_grad = contract(cotangent, down_weight, 1, 1)
    pre_grad = (2.0 * rectified * act_grad).astype(jnp.bfloat16)
    grad_down = contract(hidden, cotangent, 0, 0)
    grad_up = contract(inputs, pre_grad, 0, 0)
    grad_inputs = contract(pre_grad, up_weight, 1, 1)
    norms_up = jnp.sum(grad_up * grad_up, axis=1)
    norms_down = jnp.sum(grad_down * grad_down, axis=1)
    return (grad_inputs, grad_up, grad_down, norms_up, norms_down)
```

```python
import jax
import jax.numpy as jnp
from jax import lax
from jax.sharding import PartitionSpec as P

NARROW = jnp.bfloat16


def contract(left, right, left_dim, right_dim):
    return lax.dot_general(
        left, right, (((left_dim,), (right_dim,)), ((), ())), preferred_element_type=jnp.float32
    )


def own_rows(block, axis):
    rows = block.shape[0] // lax.axis_size(axis)
    return lax.dynamic_slice_in_dim(block, lax.axis_index(axis) * rows, rows, 0)


def exchange(blocks, axis):
    return lax.all_to_all(blocks, axis, 0, 0)


def scatter_sum(blocks, axis):
    return jnp.sum(exchange(blocks.astype(NARROW), axis).astype(jnp.float32), axis=0)


def token_plan(inputs, cotangent, up_weight, down_weight):
    reps, groups, cores = (lax.axis_size(axis) for axis in ("rep", "fs", "tp"))
    rows, width = inputs.shape
    depth, units = up_weight.shape
    mine = units // groups
    part = depth // reps

    up = exchange(up_weight.reshape(depth, groups, mine).transpose(1, 0, 2), "fs")
    up = up.reshape(width, mine)
    down = exchange(down_weight.reshape(groups, mine, depth), "fs")
    down = down.transpose(1, 0, 2).reshape(mine, width)
    tokens = lax.all_gather(own_rows(inputs, "tp"), ("fs", "tp"), axis=0, tiled=True)
    cot = lax.all_gather(own_rows(cotangent, "tp"), ("fs", "tp"), axis=0, tiled=True)

    pre_act = contract(tokens, up, 1, 0)
    act_grad = contract(cot, down, 1, 1)
    rectified = jnp.maximum(pre_act, 0.0)
    hidden = (rectified * rectified).astype(jnp.bfloat16)
    pre_grad = (2.0 * rectified * act_grad).astype(jnp.bfloat16)

    share = contract(pre_grad, up, 1, 1)
    share = share.reshape(groups, cores, rows // cores, width).transpose(1, 0, 2, 3)
    share = scatter_sum(share, "tp")
    share = scatter_sum(share, "fs")
    grad_inputs = lax.all_gather(share, "tp", axis=0, tiled=True)

    def whole_gradient(term):
        term = term.reshape(groups, reps, part, mine).transpose(1, 0, 2, 3)
        term = scatter_sum(term, "rep")
        term = exchange(term.astype(NARROW), "fs")
        term = lax.all_gather(term, "rep", axis=0)
        return term.transpose(0, 2, 1, 3).reshape(depth, units).astype(jnp.float32)

    grad_up = whole_gradient(contract(tokens, pre_grad, 0, 0))
    down_turned = whole_gradient(contract(cot, hidden, 0, 0))
    norms_up = lax.psum(jnp.sum(grad_up * grad_up, axis=1), "tp")
    norms_down = lax.psum(jnp.sum(down_turned * down_turned, axis=0), "fs")
    return (grad_inputs, grad_up, down_turned.T, norms_up, norms_down)


def weight_plan(inputs, cotangent, up_weight, down_weight):
    up_whole = lax.all_gather(up_weight, "fs", axis=0, tiled=True)
    pre_act = jnp.dot(inputs, up_whole, preferred_element_type=jnp.float32)
    act_grad = contract(cotangent, lax.all_gather(down_weight, "fs", axis=1, tiled=True), 1, 1)
    rectified = jnp.maximum(pre_act, 0.0)
    hidden = (rectified * rectified).astype(jnp.bfloat16)
    pre_grad = (2.0 * rectified * act_grad).astype(jnp.bfloat16)
    up_part = lax.psum_scatter(
        contract(inputs, pre_grad, 0, 0), "fs", scatter_dimension=0, tiled=True
    )
    down_part = lax.psum_scatter(
        contract(cotangent, hidden, 0, 0), "fs", scatter_dimension=0, tiled=True
    )
    grad_up, down_turned = lax.psum((up_part, down_part), "rep")
    grad_inputs = lax.psum(contract(pre_grad, up_whole, 1, 1), "tp")
    norms_up = lax.psum(jnp.sum(grad_up * grad_up, axis=1), "tp")
    norms_down = lax.psum(jnp.sum(down_turned * down_turned, axis=0), "fs")
    grad_down = down_turned.T
    return (grad_inputs, grad_up, grad_down, norms_up, norms_down)


def shards(inputs, cotangent, up_weight, down_weight):
    tokens = inputs.size * lax.axis_size("fs") // lax.axis_size("tp")
    weights = up_weight.size * lax.axis_size("fs")
    plan = token_plan if tokens <= weights else weight_plan
    return plan(inputs, cotangent, up_weight, down_weight)


def solution(mesh):
    return jax.shard_map(
        shards,
        mesh=mesh,
        in_specs=(P(("rep", "fs"), None), P(("rep", "fs"), None), P("fs", "tp"), P("tp", "fs")),
        out_specs=(P(("rep", "fs"), None), P("fs", "tp"), P("tp", "fs"), P("fs"), P("tp")),
        check_vma=False,
    )
```

```python
import jax
import jax.numpy as jnp
from jax import lax
from jax.sharding import PartitionSpec as P

NARROW = jnp.bfloat16
CHUNKS = 2


def contract(left, right, left_dim, right_dim):
    return lax.dot_general(
        left, right, (((left_dim,), (right_dim,)), ((), ())), preferred_element_type=jnp.float32
    )


def own_block(blocks, axis, shift=0):
    size = lax.axis_size(axis)
    return lax.dynamic_index_in_dim(
        blocks, lax.rem(lax.axis_index(axis) + shift, size), 0, keepdims=False
    )


def rotate(block, axis, shift):
    size = lax.axis_size(axis)
    return lax.ppermute(block, axis, [(at, (at + shift) % size) for at in range(size)])


def scatter_sum(blocks, axis):
    total = own_block(blocks, axis)
    for shift in range(1, lax.axis_size(axis)):
        sent = own_block(blocks, axis, shift).astype(NARROW)
        total = total + rotate(sent, axis, shift).astype(jnp.float32)
    return total


def gather_blocks(block, axis):
    size = lax.axis_size(axis)
    me = lax.axis_index(axis)
    held = [block] + [rotate(block, axis, shift) for shift in range(1, size)]
    placed = []
    for at in range(size):
        pick = held[0]
        for shift in range(1, size):
            pick = jnp.where(lax.rem(me - at + size, size) == shift, held[shift], pick)
        placed.append(pick)
    return jnp.stack(placed)


def fs_sum(blocks):
    groups = lax.axis_size("fs")
    pair = 2 if groups % 2 == 0 else 1
    far = groups // pair
    me = lax.axis_index("fs")
    blocks = blocks.reshape((far, pair) + blocks.shape[1:])

    def near_block(shift):
        return lax.dynamic_index_in_dim(
            blocks, lax.rem(lax.rem(me, pair) + shift, pair), 1, keepdims=False
        )

    held = near_block(0)
    for shift in range(1, pair):
        perm = [(at, at - at % pair + (at + shift) % pair) for at in range(groups)]
        got = lax.ppermute(near_block(shift).astype(NARROW), "fs", perm)
        held = held + got.astype(jnp.float32)

    def far_block(shift):
        return lax.dynamic_index_in_dim(held, lax.rem(me // pair + shift, far), 0, keepdims=False)

    total = far_block(0)
    for shift in range(1, far):
        perm = [(at, (at + shift * pair) % groups) for at in range(groups)]
        got = lax.ppermute(far_block(shift).astype(NARROW), "fs", perm)
        total = total + got.astype(jnp.float32)
    return total


def exchange(blocks, axis):
    return lax.all_to_all(blocks, axis, 0, 0)


def small_sum(value, axis):
    size = lax.axis_size(axis)
    if size & (size - 1):
        return lax.psum(value, axis)
    bit = 1
    while bit < size:
        value = value + lax.ppermute(value, axis, [(at, at ^ bit) for at in range(size)])
        bit *= 2
    return value


def token_plan(inputs, cotangent, up_weight, down_weight):
    reps, groups, cores = (lax.axis_size(axis) for axis in ("rep", "fs", "tp"))
    rows, width = inputs.shape
    depth, units = up_weight.shape
    mine = units // groups
    part = depth // reps
    half = width // cores

    few = mine // reps
    up = own_block(up_weight.reshape(reps, part, groups, mine).transpose(0, 2, 1, 3), "rep")
    down = own_block(down_weight.reshape(groups, reps, few, depth).transpose(1, 0, 2, 3), "rep")
    both = jnp.concatenate([up, down.reshape(groups, part, mine)], axis=1)
    both = gather_blocks(exchange(both, "fs"), "rep")
    up = both[:, :, :part].transpose(1, 0, 2, 3).reshape(width, mine)
    down = both[:, :, part:].reshape(reps, groups, few, depth)
    down = down.transpose(0, 2, 1, 3).reshape(mine, width)
    tokens = lax.all_gather(
        own_block(inputs.reshape(cores, rows // cores, width), "tp"), ("fs", "tp"), axis=0, tiled=True
    )
    cot = lax.all_gather(
        own_block(cotangent.reshape(cores, rows // cores, width), "tp"), ("fs", "tp"), axis=0, tiled=True
    )

    pre_act = contract(tokens, up, 1, 0)
    act_grad = contract(cot, down, 1, 1)
    rectified = jnp.maximum(pre_act, 0.0)
    hidden = (rectified * rectified).astype(jnp.bfloat16)
    pre_grad = (2.0 * rectified * act_grad).astype(jnp.bfloat16)

    up_rows = up.reshape(cores, half, mine)
    share = contract(pre_grad, own_block(up_rows, "tp"), 1, 1)
    for shift in range(1, cores):
        sent = contract(pre_grad, own_block(up_rows, "tp", shift), 1, 1).astype(NARROW)
        share = share + rotate(sent, "tp", shift).astype(jnp.float32)
    chunks = CHUNKS if half % (128 * CHUNKS) == 0 else 1
    share = share.reshape(groups, rows, half)
    step = half // chunks
    share = jnp.concatenate(
        [fs_sum(share[:, :, at * step : (at + 1) * step]) for at in range(chunks)], axis=1
    )
    share = gather_blocks(share, "tp")
    grad_inputs = share.transpose(1, 0, 2).reshape(rows, width)

    def spread(term):
        term = term.reshape(groups, reps, part, mine).transpose(1, 0, 2, 3)
        return exchange(scatter_sum(term, "rep").astype(NARROW), "fs")

    def whole(term):
        term = gather_blocks(term, "rep")
        return term.transpose(0, 2, 1, 3).reshape(depth, units).astype(jnp.float32)

    down_turned = whole(spread(contract(cot, hidden, 0, 0)))
    grad_up = whole(spread(contract(tokens, pre_grad, 0, 0)))
    norms_up = small_sum(jnp.sum(grad_up * grad_up, axis=1), "tp")
    norms_down = small_sum(jnp.sum(down_turned * down_turned, axis=0), "fs")
    return (grad_inputs, grad_up, down_turned.T, norms_up, norms_down)


def weight_plan(inputs, cotangent, up_weight, down_weight):
    up_whole = lax.all_gather(up_weight, "fs", axis=0, tiled=True)
    pre_act = jnp.dot(inputs, up_whole, preferred_element_type=jnp.float32)
    act_grad = contract(cotangent, lax.all_gather(down_weight, "fs", axis=1, tiled=True), 1, 1)
    rectified = jnp.maximum(pre_act, 0.0)
    hidden = (rectified * rectified).astype(jnp.bfloat16)
    pre_grad = (2.0 * rectified * act_grad).astype(jnp.bfloat16)
    up_part = lax.psum_scatter(
        contract(inputs, pre_grad, 0, 0), "fs", scatter_dimension=0, tiled=True
    )
    down_part = lax.psum_scatter(
        contract(cotangent, hidden, 0, 0), "fs", scatter_dimension=0, tiled=True
    )
    grad_up, down_turned = lax.psum((up_part, down_part), "rep")
    grad_inputs = lax.psum(contract(pre_grad, up_whole, 1, 1), "tp")
    norms_up = lax.psum(jnp.sum(grad_up * grad_up, axis=1), "tp")
    norms_down = lax.psum(jnp.sum(down_turned * down_turned, axis=0), "fs")
    grad_down = down_turned.T
    return (grad_inputs, grad_up, grad_down, norms_up, norms_down)


def shards(inputs, cotangent, up_weight, down_weight):
    tokens = inputs.size * lax.axis_size("fs") // lax.axis_size("tp")
    weights = up_weight.size * lax.axis_size("fs")
    plan = token_plan if tokens <= weights else weight_plan
    return plan(inputs, cotangent, up_weight, down_weight)


def solution(mesh):
    return jax.shard_map(
        shards,
        mesh=mesh,
        in_specs=(P(("rep", "fs"), None), P(("rep", "fs"), None), P("fs", "tp"), P("tp", "fs")),
        out_specs=(P(("rep", "fs"), None), P("fs", "tp"), P("tp", "fs"), P("fs"), P("tp")),
        check_vma=False,
    )
```

```python
import jax
import jax.numpy as jnp
from jax import lax
from jax.sharding import PartitionSpec as P

NARROW = jnp.bfloat16
CHUNKS = 2


def contract(left, right, left_dim, right_dim):
    return lax.dot_general(
        left, right, (((left_dim,), (right_dim,)), ((), ())), preferred_element_type=jnp.float32
    )


def own_block(blocks, axis, shift=0):
    size = lax.axis_size(axis)
    return lax.dynamic_index_in_dim(
        blocks, lax.rem(lax.axis_index(axis) + shift, size), 0, keepdims=False
    )


def rotate(block, axis, shift):
    size = lax.axis_size(axis)
    return lax.ppermute(block, axis, [(at, (at + shift) % size) for at in range(size)])


def scatter_sum(blocks, axis):
    total = own_block(blocks, axis)
    for shift in range(1, lax.axis_size(axis)):
        sent = own_block(blocks, axis, shift).astype(NARROW)
        total = total + rotate(sent, axis, shift).astype(jnp.float32)
    return total


def gather_blocks(block, axis):
    size = lax.axis_size(axis)
    me = lax.axis_index(axis)
    held = [block] + [rotate(block, axis, shift) for shift in range(1, size)]
    placed = []
    for at in range(size):
        pick = held[0]
        for shift in range(1, size):
            pick = jnp.where(lax.rem(me - at + size, size) == shift, held[shift], pick)
        placed.append(pick)
    return jnp.stack(placed)


def fs_sum(blocks, ahead=None):
    groups = lax.axis_size("fs")
    pair = 2 if groups % 2 == 0 else 1
    far = groups // pair
    me = lax.axis_index("fs")
    blocks = blocks.reshape((far, pair) + blocks.shape[1:])

    def near_block(shift):
        return lax.dynamic_index_in_dim(
            blocks, lax.rem(lax.rem(me, pair) + shift, pair), 1, keepdims=False
        )

    held = near_block(0)
    for shift in range(1, pair):
        perm = [(at, at - at % pair + (at + shift) % pair) for at in range(groups)]
        got = lax.ppermute(near_block(shift).astype(NARROW), "fs", perm)
        held = held + got.astype(jnp.float32)

    if ahead is not None:
        held, ahead = lax.optimization_barrier((held, ahead))

    def far_block(shift):
        return lax.dynamic_index_in_dim(held, lax.rem(me // pair + shift, far), 0, keepdims=False)

    total = far_block(0)
    for shift in range(1, far):
        perm = [(at, (at + shift * pair) % groups) for at in range(groups)]
        got = lax.ppermute(far_block(shift).astype(NARROW), "fs", perm)
        total = total + got.astype(jnp.float32)
    return total, ahead


def exchange(blocks, axis):
    return lax.all_to_all(blocks, axis, 0, 0)


def small_sum(value, axis):
    size = lax.axis_size(axis)
    if size & (size - 1):
        return lax.psum(value, axis)
    bit = 1
    while bit < size:
        value = value + lax.ppermute(value, axis, [(at, at ^ bit) for at in range(size)])
        bit *= 2
    return value


def token_plan(inputs, cotangent, up_weight, down_weight):
    reps, groups, cores = (lax.axis_size(axis) for axis in ("rep", "fs", "tp"))
    rows, width = inputs.shape
    depth, units = up_weight.shape
    mine = units // groups
    part = depth // reps
    half = width // cores

    few = mine // reps
    up = own_block(up_weight.reshape(reps, part, groups, mine).transpose(0, 2, 1, 3), "rep")
    down = own_block(down_weight.reshape(groups, reps, few, depth).transpose(1, 0, 2, 3), "rep")
    both = jnp.concatenate([up, down.reshape(groups, part, mine)], axis=1)
    both = gather_blocks(exchange(both, "fs"), "rep")
    up = both[:, :, :part].transpose(1, 0, 2, 3).reshape(width, mine)
    down = both[:, :, part:].reshape(reps, groups, few, depth)
    down = down.transpose(0, 2, 1, 3).reshape(mine, width)
    tokens = lax.all_gather(
        own_block(inputs.reshape(cores, rows // cores, width), "tp"), ("fs", "tp"), axis=0, tiled=True
    )
    cot = lax.all_gather(
        own_block(cotangent.reshape(cores, rows // cores, width), "tp"), ("fs", "tp"), axis=0, tiled=True
    )

    pre_act = contract(tokens, up, 1, 0)
    act_grad = contract(cot, down, 1, 1)
    rectified = jnp.maximum(pre_act, 0.0)
    hidden = (rectified * rectified).astype(jnp.bfloat16)
    pre_grad = (2.0 * rectified * act_grad).astype(jnp.bfloat16)

    up_rows = up.reshape(cores, half, mine)
    share = contract(pre_grad, own_block(up_rows, "tp"), 1, 1)
    for shift in range(1, cores):
        sent = contract(pre_grad, own_block(up_rows, "tp", shift), 1, 1).astype(NARROW)
        share = share + rotate(sent, "tp", shift).astype(jnp.float32)
    chunks = CHUNKS if half % (128 * CHUNKS) == 0 else 1
    share = share.reshape(groups, rows, half)
    step = half // chunks
    def spread(term):
        term = term.reshape(groups, reps, part, mine).transpose(1, 0, 2, 3)
        return exchange(scatter_sum(term, "rep").astype(NARROW), "fs")

    def whole(term):
        term = gather_blocks(term, "rep")
        return term.transpose(0, 2, 1, 3).reshape(depth, units).astype(jnp.float32)

    spreads = (spread(contract(cot, hidden, 0, 0)), spread(contract(tokens, pre_grad, 0, 0)))
    sums = []
    for at in range(chunks):
        ahead = spreads if at == chunks - 1 else None
        total, ahead = fs_sum(share[:, :, at * step : (at + 1) * step], ahead)
        sums.append(total)
    share = jnp.concatenate(sums, axis=1)
    share = gather_blocks(share, "tp")
    grad_inputs = share.transpose(1, 0, 2).reshape(rows, width)

    down_turned, grad_up = whole(ahead[0]), whole(ahead[1])
    norms_up = small_sum(jnp.sum(grad_up * grad_up, axis=1), "tp")
    norms_down = small_sum(jnp.sum(down_turned * down_turned, axis=0), "fs")
    return (grad_inputs, grad_up, down_turned.T, norms_up, norms_down)


def weight_plan(inputs, cotangent, up_weight, down_weight):
    up_whole = lax.all_gather(up_weight, "fs", axis=0, tiled=True)
    pre_act = jnp.dot(inputs, up_whole, preferred_element_type=jnp.float32)
    act_grad = contract(cotangent, lax.all_gather(down_weight, "fs", axis=1, tiled=True), 1, 1)
    rectified = jnp.maximum(pre_act, 0.0)
    hidden = (rectified * rectified).astype(jnp.bfloat16)
    pre_grad = (2.0 * rectified * act_grad).astype(jnp.bfloat16)
    up_part = lax.psum_scatter(
        contract(inputs, pre_grad, 0, 0), "fs", scatter_dimension=0, tiled=True
    )
    down_part = lax.psum_scatter(
        contract(cotangent, hidden, 0, 0), "fs", scatter_dimension=0, tiled=True
    )
    grad_up, down_turned = lax.psum((up_part, down_part), "rep")
    grad_inputs = lax.psum(contract(pre_grad, up_whole, 1, 1), "tp")
    norms_up = lax.psum(jnp.sum(grad_up * grad_up, axis=1), "tp")
    norms_down = lax.psum(jnp.sum(down_turned * down_turned, axis=0), "fs")
    grad_down = down_turned.T
    return (grad_inputs, grad_up, grad_down, norms_up, norms_down)


def shards(inputs, cotangent, up_weight, down_weight):
    tokens = inputs.size * lax.axis_size("fs") // lax.axis_size("tp")
    weights = up_weight.size * lax.axis_size("fs")
    plan = token_plan if tokens <= weights else weight_plan
    return plan(inputs, cotangent, up_weight, down_weight)


def solution(mesh):
    return jax.shard_map(
        shards,
        mesh=mesh,
        in_specs=(P(("rep", "fs"), None), P(("rep", "fs"), None), P("fs", "tp"), P("tp", "fs")),
        out_specs=(P(("rep", "fs"), None), P("fs", "tp"), P("tp", "fs"), P("fs"), P("tp")),
        check_vma=False,
    )
```
